32 devices in a mesh: rep: 2 (over x), fs: 8 (over z, y), tp: 2 (over core).
Axes of the slice: x: 2, y: 2, z: 4, core: 2. Of those that a mesh axis runs over, the one named last changes fastest.
Arguments:
- tokens: bfloat16 [12288, 2048], P(('rep', 'fs')), may hold values from -6 to 6
- norm_gain: float32 [2048], replicated, may hold values from 0.1 to 1.9
- up_weight: bfloat16 [2048, 8192], P('fs', 'tp'), may hold values from -0.125 to 0.125
- down_weight: bfloat16 [8192, 2048], P('tp', 'fs'), may hold values from -0.0625 to 0.0625
Outputs:
- layer_out: bfloat16 [12288, 2048], P(('rep', 'fs'), 'tp')
The draws below stay inside these ranges and needn't reach their ends.
All inputs are finite; a program needn't handle non-finite values.
Results may differ from the reference program's by a relative error of at most 0.013.
Values may be sent and summed in bfloat16 or wider, within the bound.
A program may use at most 128 MiB of HBM per device.

```python
import jax
import jax.numpy as jnp
from jax import lax

D = 2048
FF = 8192
TOK_GRP = 768
TOKENS = 12288
N_REP = 2
N_FS = 8
N_TP = 2


def block_scale(own_key, extent, split, smallest, high):
    gain, own = 1.0, jax.random.fold_in(own_key, 6)
    for dim, parts in split:
        draws = jnp.exp(jax.random.uniform(jax.random.fold_in(own, dim), (parts,), jnp.float32, smallest / len(split), high / len(split)))
        gain = gain * jnp.repeat(draws, extent[dim] // parts).reshape([-1 if axis == dim else 1 for axis in range(len(extent))])
    return gain


def gaussian(key, shape, scale, bound, cuts=(), dtype=jnp.bfloat16):
    entries = jax.random.normal(key, shape, jnp.float32) * scale
    if len(cuts) > 0:
        entries = block_scale(key, shape, cuts, -0.22, 0.18) * entries
    return jnp.clip(entries, min=-bound, max=bound).astype(dtype)


def setup_inputs(seed: int = 0) -> dict:
    seeds = jax.random.split(jax.random.key(seed), 5)
    return {
        "tokens": gaussian(seeds[0], (TOKENS, D), 1.0, 6.0, ((0, 16),)),
        "norm_gain": jnp.clip(1.0 + 0.18 * jax.random.normal(seeds[1], (D,), jnp.float32), 0.1, 1.9),
        "up_weight": gaussian(seeds[2], (D, FF), D ** -0.5, 0.125, ((0, 8), (1, 2))),
        "down_weight": gaussian(seeds[3], (FF, D), FF ** -0.5, 0.0625, ((0, 2), (1, 8))),
    }


def group_layer(rows, norm_gain, up_weight, down_weight):
    xf = rows.astype(jnp.float32)
    inv_rms = lax.rsqrt(lax.optimization_barrier(jnp.mean(xf * xf, axis=-1, keepdims=True)) + 1e-06)
    normed = (xf * inv_rms * norm_gain).astype(jnp.bfloat16)
    pre = jnp.dot(normed, up_weight, preferred_element_type=jnp.float32)
    hidden = jnp.square(jax.nn.relu(pre)).astype(jnp.bfloat16)
    width = hidden.shape[1] // N_TP
    total = xf
    for block in range(N_TP):
        partial_value = jnp.dot(hidden[:, block * width:(block + 1) * width], down_weight[block * width:(block + 1) * width], preferred_element_type=jnp.float32)
        total = total + partial_value.astype(jnp.bfloat16).astype(jnp.float32)
    return total.astype(jnp.bfloat16)

def reference(tokens, norm_gain, up_weight, down_weight):
    groups = tokens.reshape(N_REP * N_FS, TOK_GRP, D)
    result = lax.map(lambda rows: group_layer(rows, norm_gain, up_weight, down_weight), groups)
    return result.reshape(TOKENS, D)
```

```python
import functools

import jax
import jax.numpy as jnp
from jax import lax
from jax.experimental import pallas as pl
from jax.experimental.pallas import tpu as pltpu
from jax.sharding import PartitionSpec as P

MESH = pl.DeviceIdType.MESH
F32 = jnp.float32
BF16 = jnp.bfloat16


CHUNKS = 4
FORWARD_A = (3,)


def kernel(nz, eps, tokens, gain, up, down, out, T, acc, hid, U, Dn, Pr, Ar, Br, tokv, gv, loc,
           tok_s, tok_r, wu_s, wu_r, wd_s, wd_r, zu_s, zu_r, zd_s, zd_r, d_s, d_r, a_s, a_r, b_s, b_r,
           f_s, f_r):
    x, f, c = lax.axis_index("rep"), lax.axis_index("fs"), lax.axis_index("tp")
    z, y = f // 2, f % 2
    half, blk = T.shape[3], T.shape[4]
    wide = U.shape[2]
    row = blk // 2
    sub = row // 2
    own = x * 2 + y
    ax, ay = (x + 1 - c) % 2, (y + c) % 2
    bx, by = (x + c) % 2, (y + 1 - c) % 2
    q_a, q_b, q_ab = ax * 2 + ay, bx * 2 + by, (1 - x) * 2 + 1 - y
    to_a = {"rep": ax, "fs": z * 2 + ay}
    to_b = {"rep": bx, "fs": z * 2 + by}
    to_y = {"fs": z * 2 + 1 - y}
    to_x = {"rep": 1 - x}
    to_c = {"tp": 1 - c}
    above = {"fs": jnp.minimum(z + 1, nz - 1) * 2 + y}
    below = {"fs": jnp.maximum(z - 1, 0) * 2 + y}
    has_above, has_below = z < nz - 1, z > 0
    inner = jnp.logical_and(has_above, has_below)
    edge = jnp.logical_not(inner)

    def remote(src, dst, s, r, dev):
        return pltpu.make_async_remote_copy(
            src_ref=src, dst_ref=dst, send_sem=s, recv_sem=r, device_id=dev, device_id_type=MESH)

    def order(s):
        m = jnp.minimum(z, nz - 1 - z)
        near = z - (s + 1) // 2 if s % 2 else z + s // 2
        far = jnp.where(z < nz - 1 - z, s, nz - 1 - s)
        return jnp.where(s <= 2 * m, near, far)

    barrier = pltpu.get_barrier_semaphore()
    for dev in (to_x, to_y, to_c):
        pl.semaphore_signal(barrier, inc=1, device_id=dev, device_id_type=MESH)

    @pl.when(has_above)
    def _():
        pl.semaphore_signal(barrier, inc=1, device_id=above, device_id_type=MESH)

    @pl.when(has_below)
    def _():
        pl.semaphore_signal(barrier, inc=1, device_id=below, device_id_type=MESH)

    def up_part(q, k, n):
        return up.at[pl.ds(k * sub, n * sub), pl.ds(pl.multiple_of(q * wide, wide), wide)]

    def down_part(q):
        return down.at[pl.ds(pl.multiple_of(q * wide, wide), wide)]

    part = row // 2
    parts = ((0, row), (row, part), (row + part, part))

    def up_slot(zz, p, n=1):
        return U.at[zz, pl.ds(pl.multiple_of(p * sub, sub), n * sub)]

    def down_half(zz, p):
        return Dn.at[zz, :, pl.ds(pl.multiple_of(p * row, row), row)]

    def down_slot(zz, j):
        return Dn.at[zz, :, pl.ds(*parts[j])]

    load_up = pltpu.make_async_copy(up_part(own, 0, 2), up_slot(z, 2 * y, 2), loc.at[0])
    load_down = pltpu.make_async_copy(down_part(own), down_half(z, y), loc.at[1])
    load_gain = pltpu.make_async_copy(gain, gv, loc.at[2])
    load_tok = [pltpu.make_async_copy(
        tokens.at[pl.ds(pl.multiple_of(h * half, half), half)], tokv.at[h], loc.at[3 + i])
        for i, h in enumerate((c, 1 - c))]
    load_up.start()
    load_gain.start()
    for copy in load_tok:
        copy.start()
    load_down.start()
    pl.semaphore_wait(barrier, 3 + jnp.where(has_above, 1, 0) + jnp.where(has_below, 1, 0))

    up_order = (2 * y, 2 * y + 1, 2 * (1 - y), 2 * (1 - y) + 1)
    swap_up = [remote(up_part(x * 2 + 1 - y, k, 1), up_slot(z, 2 * y + k), wu_s.at[k], wu_r.at[k], to_y)
               for k in range(2)]
    swap_down = remote(down_part(x * 2 + 1 - y), down_half(z, y), wd_s.at[0], wd_r.at[0], to_y)

    def hop(w, upward, zz, p):
        slot, s, r = ((up_slot, zu_s, zu_r), (down_slot, zd_s, zd_r))[w]
        return remote(slot(zz, p), slot(zz, p), s.at[0 if upward else 1, zz, p],
                      r.at[zz, p], above if upward else below)

    def send(w, zz, p, act="start"):
        @pl.when(jnp.logical_and(has_above, zz <= z))
        def _():
            hop(w, True, zz, p).start() if act == "start" else hop(w, True, zz, p).wait_send()

        @pl.when(jnp.logical_and(has_below, zz >= z))
        def _():
            hop(w, False, zz, p).start() if act == "start" else hop(w, False, zz, p).wait_send()

    def relay(w, s, p):
        zz = order(s)

        @pl.when(inner)
        def _():
            hop(w, True, zz, p).wait_recv()
        send(w, zz, p)

    def arrived(w, s, p):
        @pl.when(edge)
        def _():
            hop(w, True, order(s), p).wait_recv()

    few = half // CHUNKS

    def piece(q, r):
        return T.at[:, q, c, pl.ds(r * few, few)]

    def tok(kind, r):
        if kind < 2:
            src, dev = piece(own, r), (to_a, to_b)[kind]
        elif kind == 2:
            flip = jnp.logical_and(c == 0, r in FORWARD_A)
            src = piece(jnp.where(flip, q_b, q_a), r)
            dev = {"rep": jnp.where(flip, ax, bx), "fs": z * 2 + jnp.where(flip, ay, by)}
        else:
            src, dev = piece((q_a, q_b, q_ab)[kind - 3], r), to_c
        return remote(src, src, tok_s.at[kind, r], tok_r.at[kind, r], dev)

    def norm(h, first, last):
        step = 16

        @pl.loop(first // step, last // step)
        def _(i):
            r = pl.ds(pl.multiple_of(i * step, step), step)
            xf = tokv[h, r, :].astype(F32)
            inv = lax.rsqrt(jnp.mean(xf * xf, axis=-1, keepdims=True) + eps)
            normed = (xf * inv * gv[...]).astype(BF16)
            for k in range(nz):
                T[k, own, h, r, :] = normed[:, k * blk:(k + 1) * blk]

    def up_blocks(blocks, s):
        zz = order(s)

        @pl.loop(0, 2 * len(blocks))
        def _(i):
            q, h = blocks[0], i % 2
            for n in range(1, len(blocks)):
                q = jnp.where(i // 2 == n, blocks[n], q)
            term = jnp.dot(T[zz, q, h], U[zz], preferred_element_type=F32)
            if s > 0:
                term += acc[q, h]
            if s < nz - 1:
                acc[q, h] = term
            else:
                hid[q, h] = jnp.square(jnp.maximum(term, 0.0)).astype(BF16)

    load_up.wait()
    for p in up_order[:2]:
        send(0, z, p)
    for copy in swap_up:
        copy.start()
    load_gain.wait()
    load_tok[0].wait()
    for r in range(CHUNKS):
        norm(c, r * few, (r + 1) * few)
        tok(0, r).start()
        tok(1, r).start()
    load_tok[1].wait()
    norm(1 - c, 0, half)
    for k in range(2):
        swap_up[k].wait_recv()
        send(0, z, up_order[2 + k])
    for p in up_order:
        for s in range(1, min(3, nz)):
            relay(0, s, p)
    up_blocks((own,), 0)
    rest = [(s, p) for s in range(3, nz) for p in up_order]
    for r in range(CHUNKS):
        for kind in range(2):
            tok(kind, r).wait_recv()
            tok(3 + kind, r).start()
        tok(2, r).start()
        for s, p in rest[r::CHUNKS]:
            relay(0, s, p)
    load_down.wait()
    swap_down.start()

    def send_half(p):
        @pl.when(p == 0)
        def _():
            send(1, z, 0)

        @pl.when(p == 1)
        def _():
            send(1, z, 1)
            send(1, z, 2)

    send_half(y)

    def edge_up(s):
        for p in up_order:
            arrived(0, s, p)

    edge_up(1)
    up_blocks((own,), 1)
    for r in range(CHUNKS):
        tok(3, r).wait_recv()
        tok(4, r).wait_recv()
    up_blocks((q_a, q_b), 0)
    up_blocks((q_a, q_b), 1)
    for s in range(2, nz - 1):
        edge_up(s)
        up_blocks((own, q_a, q_b), s)

    @pl.when(inner)
    def _():
        up_blocks((own, q_a, q_b), nz - 1)
    for r in range(CHUNKS):
        tok(2, r).wait_recv()
        tok(5, r).start()
    for r in range(CHUNKS):
        tok(5, r).wait_recv()
    for s in range(nz - 1):
        up_blocks((q_ab,), s)
    edge_up(nz - 1)

    @pl.when(inner)
    def _():
        up_blocks((q_ab,), nz - 1)

    @pl.when(edge)
    def _():
        up_blocks((own, q_a, q_b, q_ab), nz - 1)
    swap_down.wait_recv()
    send_half(1 - y)
    for r in range(CHUNKS):
        for kind in range(6):
            tok(kind, r).wait_send()

    def cols(p):
        return pl.ds(*p)

    def d2d(s, p):
        zz = order(s)
        return remote(T.at[zz, :, 1 - c, :, cols(p)], Pr.at[zz, :, :, cols(p)],
                      d_s.at[zz, tag(p)], d_r.at[zz, tag(p)], to_c)

    def to_first(s, p, i):
        zz = order(s)
        return remote(T.at[zz, (q_a, q_ab)[i], c, :, cols(p)], Ar.at[zz, i, :, cols(p)],
                      a_s.at[zz, tag(p), i], a_r.at[zz, tag(p), i], to_a)

    def to_second(s, p):
        zz = order(s)
        return remote(T.at[zz, q_b, c, :, cols(p)], Br.at[zz, :, cols(p)],
                      b_s.at[zz, tag(p)], b_r.at[zz, tag(p)], to_b)

    def place(s, p):
        k = order(s) % (nz // 2)
        return (pl.ds(pl.multiple_of(c * half, half), half),
                pl.ds(pl.multiple_of(k * blk + p[0], part), p[1]))

    def finish(s, p):
        zz = order(s)
        return remote(T.at[zz, own, c, :, cols(p)], out.at[place(s, p)],
                      f_s.at[zz, tag(p)], f_r.at[zz, tag(p)], to_c)

    def tag(p):
        return 2 if p[0] > row else p[0] // row

    def mine(s):
        return order(s) // (nz // 2) == c

    def stage_a(s, p):
        zz = order(s)
        for h in (1 - c, c):
            @pl.loop(0, 4, unroll=4)
            def _(q):
                T[zz, q, h, :, cols(p)] = jnp.dot(
                    hid[q, h], Dn[zz, :, cols(p)], preferred_element_type=F32).astype(BF16)
            if h is not c:
                d2d(s, p).start()

    def stage_b(s, p):
        zz, k = order(s), cols(p)
        d2d(s, p).wait_recv()
        for i, q in ((1, q_ab), (0, q_a), (2, q_b), (3, own)):
            T[zz, q, c, :, k] = (
                T[zz, q, c, :, k].astype(F32) + Pr[zz, q, :, k].astype(F32)).astype(BF16)
            if i < 2:
                to_first(s, p, i).start()

    def stage_c(s, p):
        zz, k = order(s), cols(p)
        to_first(s, p, 1).wait_recv()
        T[zz, q_b, c, :, k] = (
            T[zz, q_b, c, :, k].astype(F32) + Ar[zz, 1, :, k].astype(F32)).astype(BF16)
        to_second(s, p).start()

    def stage_d(s, p):
        zz, k = order(s), cols(p)
        to_first(s, p, 0).wait_recv()
        to_second(s, p).wait_recv()
        total = (tokv[c, :, pl.ds(pl.multiple_of(zz * blk + p[0], part), p[1])].astype(F32)
                 + T[zz, own, c, :, k].astype(F32) + Ar[zz, 0, :, k].astype(F32)
                 + Br[zz, :, k].astype(F32)).astype(BF16)

        @pl.when(mine(s))
        def _():
            out[place(s, p)] = total

        @pl.when(jnp.logical_not(mine(s)))
        def _():
            T[zz, own, c, :, k] = total
            finish(s, p).start()

    steps = [(s, p) for s in range(nz) for p in ((0, row), (row, row))]
    steps[-1:] = [(nz - 1, p) for p in parts[1:]]
    needs = [[j for j in range(3) if p[0] <= parts[j][0] < sum(p)] for _, p in steps]
    flat = [(s, j) for (s, _), js in zip(steps, needs) for j in js]
    relayed = set()

    def relay_until(s, j):
        for item in flat:
            if 0 < item[0] and item not in relayed and (item[0] < s or item[0] == s and item[1] <= j):
                relayed.add(item)
                relay(1, *item)

    for n, (s, p) in enumerate(steps):
        first = tag(p) == 0
        if s == 1:
            for j in needs[n]:
                relay(1, 1, j)
                relay(1, 2, j)
            relayed.update((k, j) for k in (1, 2) for j in needs[n])
        elif s > 1:
            relay_until(*((s, needs[n][-1]) if first or s == nz - 1 else (s + 1, 0)))
        if s:
            for j in needs[n]:
                arrived(1, s, j)
        stage_a(s, p)
        if n:
            stage_c(*steps[n - 1])
        stage_b(s, p)
        if n > 1:
            stage_d(*steps[n - 2])
    stage_c(*steps[-1])
    stage_d(*steps[-2])
    stage_d(*steps[-1])

    for copy in swap_up:
        copy.wait_send()
    swap_down.wait_send()
    for s in range(nz):
        for p in up_order:
            send(0, order(s), p, "wait")
        for j in range(3):
            send(1, order(s), j, "wait")
    for s, p in steps:
        d2d(s, p).wait_send()
        to_first(s, p, 0).wait_send()
        to_first(s, p, 1).wait_send()
        to_second(s, p).wait_send()

        @pl.when(mine(s))
        def _():
            finish(s, p).wait_recv()

        @pl.when(jnp.logical_not(mine(s)))
        def _():
            finish(s, p).wait_send()


def fused(nz, tokens, gain, up, down):
    rows, d = tokens.shape
    wide = up.shape[1] // 4
    half, blk = rows // 2, d // nz
    sem = pltpu.SemaphoreType.DMA
    return pl.pallas_call(
        functools.partial(kernel, nz, 1e-06),
        out_shape=pltpu.VMEM((rows, d // 2), BF16),
        in_specs=[pl.BlockSpec(memory_space=pl.ANY)] * 4,
        out_specs=pl.BlockSpec(memory_space=pltpu.VMEM),
        scratch_shapes=[
            pltpu.VMEM((nz, 4, 2, half, blk), BF16),
            pltpu.VMEM((4, 2, half, wide), F32),
            pltpu.VMEM((4, 2, half, wide), BF16),
            pltpu.VMEM((nz, blk, wide), BF16),
            pltpu.VMEM((nz, wide, blk), BF16),
            pltpu.VMEM((nz, 4, half, blk), BF16),
            pltpu.VMEM((nz, 2, half, blk), BF16),
            pltpu.VMEM((nz, half, blk), BF16),
            pltpu.VMEM((2, half, d), BF16),
            pltpu.VMEM((1, d), F32),
            sem((5,)), sem((6, CHUNKS)), sem((6, CHUNKS)), sem((2,)), sem((2,)), sem((1,)), sem((1,)),
            sem((2, nz, 4)), sem((nz, 4)), sem((2, nz, 3)), sem((nz, 3)), sem((nz, 3)), sem((nz, 3)),
            sem((nz, 3, 2)), sem((nz, 3, 2)), sem((nz, 3)), sem((nz, 3)), sem((nz, 3)),
            sem((nz, 3)),
        ],
        compiler_params=pltpu.CompilerParams(
            collective_id=0, has_side_effects=True, vmem_limit_bytes=58 * 2**20),
    )(tokens, gain.reshape(1, d), up, down)


def spread(normed, up_weight, down_weight):
    n_rep = lax.axis_size("rep")
    rep = lax.axis_index("rep")
    ff = up_weight.shape[1] // n_rep
    up = lax.all_gather(
        lax.dynamic_slice_in_dim(up_weight, rep * ff, ff, 1), "fs", axis=0, tiled=True)
    down = lax.all_gather(
        lax.dynamic_slice_in_dim(down_weight, rep * ff, ff, 0), "fs", axis=1, tiled=True)
    normed = lax.all_gather(normed, "rep", axis=0, tiled=True)
    pre = jnp.dot(normed, up, preferred_element_type=F32)
    hidden = jnp.square(jax.nn.relu(pre)).astype(BF16)
    terms = jnp.dot(hidden, down, preferred_element_type=F32).astype(BF16)
    summed = lax.psum_scatter(terms, "tp", scatter_dimension=1, tiled=True)
    return lax.psum_scatter(summed, "rep", scatter_dimension=0, tiled=True)


def local(tokens, norm_gain, up_weight, down_weight):
    n_rep, n_fs, n_tp = (lax.axis_size(a) for a in ("rep", "fs", "tp"))
    if n_rep == 2 and n_tp == 2 and n_fs % 4 == 0:
        got = fused(n_fs // 2, tokens, norm_gain, up_weight, down_weight)
        return got
    xf = tokens.astype(F32)
    inv_rms = lax.rsqrt(jnp.mean(xf * xf, axis=-1, keepdims=True) + 1e-06)
    normed = (xf * inv_rms * norm_gain).astype(BF16)
    summed = spread(normed, up_weight, down_weight).astype(F32)
    width = summed.shape[1]
    own_cols = lax.dynamic_slice_in_dim(xf, lax.axis_index("tp") * width, width, 1)
    return (own_cols + summed).astype(BF16)


def solution(mesh):
    placed = (P(("rep", "fs"), None), P(), P("fs", "tp"), P("tp", "fs"))
    return jax.shard_map(
        local, mesh=mesh, in_specs=placed, out_specs=P(("rep", "fs"), "tp"), check_vma=False
    )
```

```python
import functools

import jax
import jax.numpy as jnp
from jax import lax
from jax.experimental import pallas as pl
from jax.experimental.pallas import tpu as pltpu
from jax.sharding import PartitionSpec as P

MESH = pl.DeviceIdType.MESH
F32 = jnp.float32
BF16 = jnp.bfloat16


CHUNKS = 4
FORWARD_A = (3,)
DEEP = 2


def kernel(nz, eps, tokens, gain, up, down, out, T, acc, hid, U, Dn, Pr, Ar, Br, P2, A2, B2, tokv, gv, loc,
           tok_s, tok_r, cor_r, w_s, w_r, z_s, zu_r, zd_r, d_r, a_r, b_r, out_s, f_r,
           e_s, e_r):
    x, f, c = lax.axis_index("rep"), lax.axis_index("fs"), lax.axis_index("tp")
    z, y = f // 2, f % 2
    half, blk = T.shape[3], T.shape[4]
    wide = U.shape[2]
    row = blk // 2
    sub = row // 2
    own = x * 2 + y
    ax, ay = (x + 1 - c) % 2, (y + c) % 2
    bx, by = (x + c) % 2, (y + 1 - c) % 2
    q_a, q_b, q_ab = ax * 2 + ay, bx * 2 + by, (1 - x) * 2 + 1 - y
    to_a = {"rep": ax, "fs": z * 2 + ay}
    to_b = {"rep": bx, "fs": z * 2 + by}
    to_y = {"fs": z * 2 + 1 - y}
    to_x = {"rep": 1 - x}
    to_c = {"tp": 1 - c}
    above = {"fs": jnp.minimum(z + 1, nz - 1) * 2 + y}
    below = {"fs": jnp.maximum(z - 1, 0) * 2 + y}
    has_above, has_below = z < nz - 1, z > 0
    inner = jnp.logical_and(has_above, has_below)
    edge = jnp.logical_not(inner)

    def remote(src, dst, s, r, dev):
        return pltpu.make_async_remote_copy(
            src_ref=src, dst_ref=dst, send_sem=s, recv_sem=r, device_id=dev, device_id_type=MESH)

    def order(s):
        m = jnp.minimum(z, nz - 1 - z)
        near = z - (s + 1) // 2 if s % 2 else z + s // 2
        far = jnp.where(z < nz - 1 - z, s, nz - 1 - s)
        return jnp.where(s <= 2 * m, near, far)

    barrier = pltpu.get_barrier_semaphore()
    for dev in (to_x, to_y, to_c):
        pl.semaphore_signal(barrier, inc=1, device_id=dev, device_id_type=MESH)

    @pl.when(has_above)
    def _():
        pl.semaphore_signal(barrier, inc=1, device_id=above, device_id_type=MESH)

    @pl.when(has_below)
    def _():
        pl.semaphore_signal(barrier, inc=1, device_id=below, device_id_type=MESH)

    def up_part(q, k, n):
        return up.at[pl.ds(k * sub, n * sub), pl.ds(pl.multiple_of(q * wide, wide), wide)]

    def down_part(q):
        return down.at[pl.ds(pl.multiple_of(q * wide, wide), wide)]

    part = row // 2
    deep = wide * DEEP // 4
    parts = ((0, row, 0, wide), (row, part, 0, wide), (row + part, part, 0, deep),
             (row + part, part, deep, wide - deep))

    def up_slot(zz, p, n=1):
        return U.at[zz, pl.ds(pl.multiple_of(p * sub, sub), n * sub)]

    def up_piece(zz, p):
        return up_slot(zz, 2 * y, 2) if p == 0 else up_slot(zz, 2 * (1 - y) + p - 1)

    def down_half(zz, p):
        return Dn.at[zz, :, pl.ds(pl.multiple_of(p * row, row), row)]

    def down_slot(zz, j):
        return Dn.at[zz, pl.ds(*parts[j][2:]), pl.ds(*parts[j][:2])]

    load_up = pltpu.make_async_copy(up_part(own, 0, 2), up_slot(z, 2 * y, 2), loc.at[0])
    load_down = pltpu.make_async_copy(down_part(own), down_half(z, y), loc.at[1])
    load_gain = pltpu.make_async_copy(gain, gv, loc.at[2])
    load_tok = [pltpu.make_async_copy(
        tokens.at[pl.ds(pl.multiple_of(h * half, half), half)], tokv.at[h], loc.at[3 + i])
        for i, h in enumerate((c, 1 - c))]
    load_up.start()
    load_gain.start()
    for copy in load_tok:
        copy.start()
    load_down.start()
    pl.semaphore_wait(barrier, 3 + jnp.where(has_above, 1, 0) + jnp.where(has_below, 1, 0))

    up_order = (0, 1, 2)
    swap_up = [remote(up_part(x * 2 + 1 - y, k, 1), up_slot(z, 2 * y + k), w_s.at[0], w_r.at[k], to_y)
               for k in range(2)]
    swap_down = remote(down_part(x * 2 + 1 - y), down_half(z, y), w_s.at[1], w_r.at[2], to_y)

    def hop(w, upward, zz, p):
        slot, r = ((up_piece, zu_r), (down_slot, zd_r))[w]
        return remote(slot(zz, p), slot(zz, p), z_s.at[0 if upward else 1, zz],
                      r.at[zz, p], above if upward else below)

    def send(w, zz, p):
        @pl.when(jnp.logical_and(has_above, zz <= z))
        def _():
            hop(w, True, zz, p).start()

        @pl.when(jnp.logical_and(has_below, zz >= z))
        def _():
            hop(w, False, zz, p).start()

    def sent(zz):
        both = U.at[pl.ds(0, 2)]

        @pl.when(jnp.logical_and(has_above, zz <= z))
        def _():
            remote(both, both, z_s.at[0, zz], zu_r.at[0, 0], above).wait_send()

        @pl.when(jnp.logical_and(has_below, zz >= z))
        def _():
            remote(both, both, z_s.at[1, zz], zu_r.at[0, 0], below).wait_send()

    def relay(w, s, p):
        zz = order(s)

        @pl.when(inner)
        def _():
            hop(w, True, zz, p).wait_recv()
        send(w, zz, p)

    def arrived(w, s, p):
        @pl.when(edge)
        def _():
            hop(w, True, order(s), p).wait_recv()

    few = half // CHUNKS

    def piece(q, r):
        return T.at[:, q, c, pl.ds(r * few, few)]

    def tok(kind, r):
        if kind < 2:
            src, dev = piece(own, r), (to_a, to_b)[kind]
        elif kind == 2:
            flip = jnp.logical_and(c == 0, r in FORWARD_A)
            src = piece(jnp.where(flip, q_b, q_a), r)
            dev = {"rep": jnp.where(flip, ax, bx), "fs": z * 2 + jnp.where(flip, ay, by)}
        else:
            src, dev = piece((q_a, q_b, q_ab)[kind - 3], r), to_c
        land = tok_r.at[kind, r] if kind < 3 else cor_r.at[kind - 3]
        return remote(src, src, tok_s.at[0], land, dev)

    def crossed(kind):
        q = T.at[:, (q_b, q_a, q_ab)[kind - 3], 1 - c]
        remote(q, q, tok_s.at[0], cor_r.at[kind - 3], to_c).wait_recv()

    def norm(h, first, last):
        step = 16

        @pl.loop(first // step, last // step)
        def _(i):
            r = pl.ds(pl.multiple_of(i * step, step), step)
            xf = tokv[h, r, :].astype(F32)
            inv = lax.rsqrt(jnp.mean(xf * xf, axis=-1, keepdims=True) + eps)
            normed = (xf * inv * gv[...]).astype(BF16)
            for k in range(nz):
                T[k, own, h, r, :] = normed[:, k * blk:(k + 1) * blk]

    def up_blocks(blocks, s):
        zz = order(s)

        @pl.loop(0, 2 * len(blocks))
        def _(i):
            q, h = blocks[0], i % 2
            for n in range(1, len(blocks)):
                q = jnp.where(i // 2 == n, blocks[n], q)
            term = jnp.dot(T[zz, q, h], U[zz], preferred_element_type=F32)
            if s > 0:
                term += acc[q, h]
            if s < nz - 1:
                acc[q, h] = term
            else:
                hid[q, h] = jnp.square(jnp.maximum(term, 0.0)).astype(BF16)

    load_up.wait()
    send(0, z, 0)
    for copy in swap_up:
        copy.start()
    load_gain.wait()
    load_tok[0].wait()
    for r in range(CHUNKS):
        norm(c, r * few, (r + 1) * few)
        tok(0, r).start()
        tok(1, r).start()
    load_tok[1].wait()
    norm(1 - c, 0, half)
    for k in range(2):
        swap_up[k].wait_recv()
        send(0, z, 1 + k)
    for p in up_order:
        for s in range(1, min(3, nz)):
            relay(0, s, p)
    up_blocks((own,), 0)
    rest = [(s, p) for s in range(3, nz) for p in up_order]
    for r in range(CHUNKS):
        for kind in range(2):
            tok(kind, r).wait_recv()
            tok(3 + kind, r).start()
        tok(2, r).start()
        for s, p in rest[r::CHUNKS]:
            relay(0, s, p)
    load_down.wait()
    swap_down.start()

    def send_half(p):
        @pl.when(p == 0)
        def _():
            send(1, z, 0)

        @pl.when(p == 1)
        def _():
            for j in range(1, len(parts)):
                send(1, z, j)

    send_half(y)

    def edge_up(s):
        for p in up_order:
            arrived(0, s, p)

    edge_up(1)
    up_blocks((own,), 1)
    crossed(3)
    crossed(4)
    up_blocks((q_a, q_b), 0)
    up_blocks((q_a, q_b), 1)
    for s in range(2, nz - 1):
        edge_up(s)
        up_blocks((own, q_a, q_b), s)

    @pl.when(inner)
    def _():
        up_blocks((own, q_a, q_b), nz - 1)
    for r in range(CHUNKS):
        tok(2, r).wait_recv()
        tok(5, r).start()
    crossed(5)
    for s in range(nz - 1):
        up_blocks((q_ab,), s)
    edge_up(nz - 1)

    @pl.when(inner)
    def _():
        up_blocks((q_ab,), nz - 1)

    @pl.when(edge)
    def _():
        up_blocks((own, q_a, q_b, q_ab), nz - 1)
    swap_down.wait_recv()
    send_half(1 - y)
    every = T.at[:, pl.ds(0, 3)]
    remote(every, every, tok_s.at[0], cor_r.at[0], to_c).wait_send()

    def cols(p):
        return pl.ds(*p)

    def step(s, p):
        return 2 * s + tag(p)

    def group(s, k):
        return k if s < nz - 1 else 4 + k

    def d2d(s, p):
        zz = order(s)
        return remote(T.at[zz, :, 1 - c, :, cols(p)], Pr.at[zz, :, :, cols(p)],
                      out_s.at[group(s, 0)], d_r.at[step(s, p)], to_c)

    def to_first(s, p, i):
        zz = order(s)
        return remote(T.at[zz, (q_a, q_ab)[i], c, :, cols(p)], Ar.at[zz, i, :, cols(p)],
                      out_s.at[group(s, 1)], (b_r, a_r)[i].at[step(s, p)], to_a)

    def to_second(s, p):
        zz = order(s)
        return remote(T.at[zz, q_b, c, :, cols(p)], Br.at[zz, :, cols(p)],
                      out_s.at[group(s, 2)], b_r.at[step(s, p)], to_b)

    def place(s, p):
        k = order(s) % (nz // 2)
        return (pl.ds(pl.multiple_of(c * half, half), half),
                pl.ds(pl.multiple_of(k * blk + p[0], part), p[1]))

    def finish(s, p):
        zz = order(s)
        return remote(T.at[zz, own, c, :, cols(p)], out.at[place(s, p)],
                      out_s.at[3], f_r.at[0], to_c)

    def tag(p):
        return 2 if p[0] > row else p[0] // row

    def mine(s):
        return order(s) // (nz // 2) == c

    def stage_a(s, p):
        zz = order(s)
        for h in (1 - c, c):
            @pl.loop(0, 4, unroll=4)
            def _(q):
                T[zz, q, h, :, cols(p)] = jnp.dot(
                    hid[q, h], Dn[zz, :, cols(p)], preferred_element_type=F32).astype(BF16)
            if h is not c:
                d2d(s, p).start()

    def stage_a_early(s, p):
        zz = order(s)
        for h in range(2):
            @pl.loop(0, 4, unroll=4)
            def _(q):
                acc[q, h, :, :p[1]] = jnp.dot(
                    hid[q, h, :, :deep], Dn[zz, :deep, cols(p)], preferred_element_type=F32)

    def stage_a_late(s, p):
        zz = order(s)
        for h in range(2):
            @pl.loop(0, 4, unroll=4)
            def _(q):
                T[zz, q, h, :, cols(p)] = (acc[q, h, :, :p[1]] + jnp.dot(
                    hid[q, h, :, deep:], Dn[zz, deep:, cols(p)], preferred_element_type=F32)).astype(BF16)

            @pl.when(c == 0)
            def _():
                gather_last(s, p, h).start()

    def side(h):
        px, py = (1 - x, y), (x, 1 - y)
        (ax, ay), (bx, by) = (px, py) if h == 0 else (py, px)
        return (ax * 2 + ay, bx * 2 + by, {"rep": ax, "fs": z * 2 + ay}, {"rep": bx, "fs": z * 2 + by})

    def gather_last(s, p, h):
        return remote(T.at[order(s), :, h, :, cols(p)], P2.at[h], e_s.at[h], e_r.at[h], to_c)

    def first_last(s, p, h, i):
        qa, _, dev, _ = side(h)
        return remote(T.at[order(s), (qa, q_ab)[i], h, :, cols(p)], A2.at[h, i],
                      e_s.at[2 + 2 * h + i], e_r.at[2 + 2 * h + i], dev)

    def second_last(s, p, h):
        _, qb, _, dev = side(h)
        return remote(T.at[order(s), qb, h, :, cols(p)], B2.at[h], e_s.at[6 + h], e_r.at[6 + h], dev)

    def out_last(s, p, h):
        return (pl.ds(h * half, half),
                pl.ds(pl.multiple_of(order(s) % (nz // 2) * blk + p[0], part), p[1]))

    def finish_last(s, p, h):
        return remote(T.at[order(s), own, h, :, cols(p)], out.at[out_last(s, p, h)],
                      e_s.at[8 + h], e_r.at[8 + h], to_c)

    def last_b(s, p):
        zz, k = order(s), cols(p)
        for h in range(2):
            gather_last(s, p, h).wait_recv()
            T[zz, q_ab, h, :, k] = (
                T[zz, q_ab, h, :, k].astype(F32) + P2[h, q_ab].astype(F32)).astype(BF16)
            first_last(s, p, h, 1).start()
            for i, q in enumerate(side(h)[:2]):
                T[zz, q, h, :, k] = (
                    T[zz, q, h, :, k].astype(F32) + P2[h, q].astype(F32)).astype(BF16)
                if i == 0:
                    first_last(s, p, h, 0).start()

    def last_c(s, p):
        zz, k = order(s), cols(p)
        for h in range(2):
            qb = side(h)[1]
            first_last(s, p, h, 1).wait_recv()
            T[zz, qb, h, :, k] = (
                T[zz, qb, h, :, k].astype(F32) + A2[h, 1].astype(F32)).astype(BF16)
            second_last(s, p, h).start()

    def last_d(s, p):
        zz, k = order(s), cols(p)
        for h in range(2):
            T[zz, own, h, :, k] = (
                T[zz, own, h, :, k].astype(F32) + P2[h, own].astype(F32)).astype(BF16)
        for h in range(2):
            first_last(s, p, h, 0).wait_recv()
            second_last(s, p, h).wait_recv()
            total = (tokv[h, :, pl.ds(pl.multiple_of(zz * blk + p[0], part), p[1])].astype(F32)
                     + T[zz, own, h, :, k].astype(F32) + A2[h, 0].astype(F32)
                     + B2[h].astype(F32)).astype(BF16)

            @pl.when(mine(s))
            def _():
                out[out_last(s, p, h)] = total

            @pl.when(jnp.logical_not(mine(s)))
            def _():
                T[zz, own, h, :, k] = total
                finish_last(s, p, h).start()

    def stage_b(s, p):
        zz, k = order(s), cols(p)
        d2d(s, p).wait_recv()
        for i, q in ((1, q_ab), (0, q_a), (2, q_b), (3, own)):
            T[zz, q, c, :, k] = (
                T[zz, q, c, :, k].astype(F32) + Pr[zz, q, :, k].astype(F32)).astype(BF16)
            if i < 2:
                to_first(s, p, i).start()

    def stage_c(s, p):
        zz, k = order(s), cols(p)
        to_first(s, p, 1).wait_recv()
        T[zz, q_b, c, :, k] = (
            T[zz, q_b, c, :, k].astype(F32) + Ar[zz, 1, :, k].astype(F32)).astype(BF16)
        to_second(s, p).start()

    def stage_d(s, p):
        zz, k = order(s), cols(p)
        two = Ar.at[zz, :, :, k]
        remote(two, two, out_s.at[1], b_r.at[step(s, p)], to_a).wait_recv()
        total = (tokv[c, :, pl.ds(pl.multiple_of(zz * blk + p[0], part), p[1])].astype(F32)
                 + T[zz, own, c, :, k].astype(F32) + Ar[zz, 0, :, k].astype(F32)
                 + Br[zz, :, k].astype(F32)).astype(BF16)

        @pl.when(mine(s))
        def _():
            out[place(s, p)] = total

        @pl.when(jnp.logical_not(mine(s)))
        def _():
            T[zz, own, c, :, k] = total
            finish(s, p).start()

    steps = [(s, p) for s in range(nz) for p in ((0, row), (row, row))]
    steps[-1:] = [(nz - 1, p[:2]) for p in parts[1:3]]
    needs = [[j for j in range(len(parts)) if p[0] <= parts[j][0] < sum(p)] for _, p in steps]
    flat = [(s, j) for (s, _), js in zip(steps, needs) for j in js]
    relayed = set()

    def relay_until(s, j):
        for item in flat:
            if 0 < item[0] and item not in relayed and (item[0] < s or item[0] == s and item[1] <= j):
                relayed.add(item)
                relay(1, *item)

    last = len(steps) - 1

    def ready(n, js):
        s = steps[n][0]
        if s:
            for j in js:
                arrived(1, s, j)

    for n, (s, p) in enumerate(steps):
        first = tag(p) == 0
        if s == 1:
            for j in needs[n]:
                relay(1, 1, j)
                relay(1, 2, j)
            relayed.update((k, j) for k in (1, 2) for j in needs[n])
        elif 1 < s and n < last:
            relay_until(*((s, needs[n][-1]) if first or s == nz - 1 else (s + 1, 0)))
        if n < last:
            ready(n, needs[n])
            stage_a(s, p)
        else:
            for j, stage in zip(needs[n], (stage_a_early, stage_a_late)):
                relay_until(s, j)
                ready(n, (j,))
                stage(s, p)
        if n and n < last:
            stage_c(*steps[n - 1])
        if n < last:
            stage_b(s, p)
        if 1 < n < last:
            stage_d(*steps[n - 2])

    @pl.when(c == 1)
    def _():
        last_b(*steps[last])
    stage_c(*steps[last - 1])
    stage_d(*steps[last - 2])

    @pl.when(c == 1)
    def _():
        last_c(*steps[last])
    stage_d(*steps[last - 1])

    @pl.when(c == 1)
    def _():
        last_d(*steps[last])
    for zz in range(nz):
        sent(zz)
    ups = up_slot(0, 0, 2)
    remote(ups, ups, w_s.at[0], w_r.at[0], to_y).wait_send()
    swap_down.wait_send()

    def all_sent(ref, k):
        remote(ref, ref, out_s.at[k], d_r.at[0], to_c).wait_send()

    for k, ref in enumerate((Pr, Ar, Br)):
        all_sent(ref.at[pl.ds(0, nz - 1)], k)
        lead = (0,) + (slice(None),) * (len(ref.shape) - 2)
        all_sent(ref.at[(*lead, pl.ds(0, blk - part))], 4 + k)
    far = mine(nz - 1)
    most = out.at[pl.ds(0, half), pl.ds(0, (nz // 2) * blk - part)]
    full = out.at[pl.ds(0, half)]

    @pl.when(far)
    def _():
        all_sent(full, 3)
        remote(most, most, out_s.at[3], f_r.at[0], to_c).wait_recv()

    @pl.when(jnp.logical_not(far))
    def _():
        all_sent(most, 3)
        remote(full, full, out_s.at[3], f_r.at[0], to_c).wait_recv()

    end = steps[last]
    for h in range(2):
        @pl.when(c == 0)
        def _():
            gather_last(*end, h).wait_send()

        @pl.when(c == 1)
        def _():
            for i in range(2):
                first_last(*end, h, i).wait_send()
            second_last(*end, h).wait_send()

        @pl.when(jnp.logical_and(c == 1, jnp.logical_not(far)))
        def _():
            finish_last(*end, h).wait_send()

        @pl.when(jnp.logical_and(c == 0, far))
        def _():
            finish_last(*end, h).wait_recv()


def fused(nz, tokens, gain, up, down):
    rows, d = tokens.shape
    wide = up.shape[1] // 4
    half, blk = rows // 2, d // nz
    sem = pltpu.SemaphoreType.DMA
    return pl.pallas_call(
        functools.partial(kernel, nz, 1e-06),
        out_shape=pltpu.VMEM((rows, d // 2), BF16),
        in_specs=[pl.BlockSpec(memory_space=pl.ANY)] * 4,
        out_specs=pl.BlockSpec(memory_space=pltpu.VMEM),
        scratch_shapes=[
            pltpu.VMEM((nz, 4, 2, half, blk), BF16),
            pltpu.VMEM((4, 2, half, wide), F32),
            pltpu.VMEM((4, 2, half, wide), BF16),
            pltpu.VMEM((nz, blk, wide), BF16),
            pltpu.VMEM((nz, wide, blk), BF16),
            pltpu.VMEM((nz, 4, half, blk), BF16),
            pltpu.VMEM((nz, 2, half, blk), BF16),
            pltpu.VMEM((nz, half, blk), BF16),
            pltpu.VMEM((2, 4, half, blk // 4), BF16),
            pltpu.VMEM((2, 2, half, blk // 4), BF16),
            pltpu.VMEM((2, half, blk // 4), BF16),
            pltpu.VMEM((2, half, d), BF16),
            pltpu.VMEM((1, d), F32),
            sem((5,)), sem((1,)), sem((3, CHUNKS)), sem((3,)), sem((2,)), sem((3,)), sem((2, nz)),
            sem((nz, 3)), sem((nz, 4)), sem((2 * nz + 1,)), sem((2 * nz + 1,)), sem((2 * nz + 1,)),
            sem((7,)), sem((1,)), sem((10,)), sem((10,)),
        ],
        compiler_params=pltpu.CompilerParams(
            collective_id=0, has_side_effects=True, vmem_limit_bytes=58 * 2**20),
    )(tokens, gain.reshape(1, d), up, down)


def spread(normed, up_weight, down_weight):
    n_rep = lax.axis_size("rep")
    rep = lax.axis_index("rep")
    ff = up_weight.shape[1] // n_rep
    up = lax.all_gather(
        lax.dynamic_slice_in_dim(up_weight, rep * ff, ff, 1), "fs", axis=0, tiled=True)
    down = lax.all_gather(
        lax.dynamic_slice_in_dim(down_weight, rep * ff, ff, 0), "fs", axis=1, tiled=True)
    normed = lax.all_gather(normed, "rep", axis=0, tiled=True)
    pre = jnp.dot(normed, up, preferred_element_type=F32)
    hidden = jnp.square(jax.nn.relu(pre)).astype(BF16)
    terms = jnp.dot(hidden, down, preferred_element_type=F32).astype(BF16)
    summed = lax.psum_scatter(terms, "tp", scatter_dimension=1, tiled=True)
    return lax.psum_scatter(summed, "rep", scatter_dimension=0, tiled=True)


def local(tokens, norm_gain, up_weight, down_weight):
    n_rep, n_fs, n_tp = (lax.axis_size(a) for a in ("rep", "fs", "tp"))
    if n_rep == 2 and n_tp == 2 and n_fs % 4 == 0:
        got = fused(n_fs // 2, tokens, norm_gain, up_weight, down_weight)
        return got
    xf = tokens.astype(F32)
    inv_rms = lax.rsqrt(jnp.mean(xf * xf, axis=-1, keepdims=True) + 1e-06)
    normed = (xf * inv_rms * norm_gain).astype(BF16)
    summed = spread(normed, up_weight, down_weight).astype(F32)
    width = summed.shape[1]
    own_cols = lax.dynamic_slice_in_dim(xf, lax.axis_index("tp") * width, width, 1)
    return (own_cols + summed).astype(BF16)


def solution(mesh):
    placed = (P(("rep", "fs"), None), P(), P("fs", "tp"), P("tp", "fs"))
    return jax.shard_map(
        local, mesh=mesh, in_specs=placed, out_specs=P(("rep", "fs"), "tp"), check_vma=False
    )
```

```python
import functools

import jax
import jax.numpy as jnp
from jax import lax
from jax.experimental import pallas as pl
from jax.experimental.pallas import tpu as pltpu
from jax.sharding import PartitionSpec as P

MESH = pl.DeviceIdType.MESH
F32 = jnp.float32
BF16 = jnp.bfloat16


CHUNKS = 4
FORWARD_A = (3,)
DEEP = 2


def kernel(nz, eps, tokens, gain, up, down, out, T, acc, hid, U, Dn, Pr, Ar, Br, P2, A2, B2, tokv, gv, loc,
           tok_s, tok_r, cor_r, w_s, w_r, z_s, zu_r, zd_r, d_r, a_r, b_r, out_s, f_r,
           e_s, e_r):
    x, f, c = lax.axis_index("rep"), lax.axis_index("fs"), lax.axis_index("tp")
    z, y = f // 2, f % 2
    half, blk = T.shape[3], T.shape[4]
    wide = U.shape[2]
    row = blk // 2
    sub = row // 2
    own = x * 2 + y
    ax, ay = (x + 1 - c) % 2, (y + c) % 2
    bx, by = (x + c) % 2, (y + 1 - c) % 2
    q_a, q_b, q_ab = ax * 2 + ay, bx * 2 + by, (1 - x) * 2 + 1 - y
    to_a = {"rep": ax, "fs": z * 2 + ay}
    to_b = {"rep": bx, "fs": z * 2 + by}
    to_y = {"fs": z * 2 + 1 - y}
    to_x = {"rep": 1 - x}
    to_c = {"tp": 1 - c}
    above = {"fs": jnp.minimum(z + 1, nz - 1) * 2 + y}
    below = {"fs": jnp.maximum(z - 1, 0) * 2 + y}
    has_above, has_below = z < nz - 1, z > 0
    inner = jnp.logical_and(has_above, has_below)
    edge = jnp.logical_not(inner)

    def remote(src, dst, s, r, dev):
        return pltpu.make_async_remote_copy(
            src_ref=src, dst_ref=dst, send_sem=s, recv_sem=r, device_id=dev, device_id_type=MESH)

    def order(s):
        m = jnp.minimum(z, nz - 1 - z)
        near = z - (s + 1) // 2 if s % 2 else z + s // 2
        far = jnp.where(z < nz - 1 - z, s, nz - 1 - s)
        return jnp.where(s <= 2 * m, near, far)

    barrier = pltpu.get_barrier_semaphore()
    for dev in (to_x, to_y, to_c):
        pl.semaphore_signal(barrier, inc=1, device_id=dev, device_id_type=MESH)

    @pl.when(has_above)
    def _():
        pl.semaphore_signal(barrier, inc=1, device_id=above, device_id_type=MESH)

    @pl.when(has_below)
    def _():
        pl.semaphore_signal(barrier, inc=1, device_id=below, device_id_type=MESH)

    def up_part(q, k, n):
        return up.at[pl.ds(k * sub, n * sub), pl.ds(pl.multiple_of(q * wide, wide), wide)]

    def down_part(q):
        return down.at[pl.ds(pl.multiple_of(q * wide, wide), wide)]

    part = row // 2
    deep = wide * DEEP // 4
    parts = ((0, row, 0, wide), (row, part, 0, wide), (row + part, part, 0, deep),
             (row + part, part, deep, wide - deep))

    def up_slot(zz, p, n=1):
        return U.at[zz, pl.ds(pl.multiple_of(p * sub, sub), n * sub)]

    def up_piece(zz, p):
        return up_slot(zz, 2 * y, 2) if p == 0 else up_slot(zz, 2 * (1 - y) + p - 1)

    def down_half(zz, p):
        return Dn.at[zz, :, pl.ds(pl.multiple_of(p * row, row), row)]

    def down_slot(zz, j):
        return Dn.at[zz, pl.ds(*parts[j][2:]), pl.ds(*parts[j][:2])]

    load_up = pltpu.make_async_copy(up_part(own, 0, 2), up_slot(z, 2 * y, 2), loc.at[0])
    load_down = pltpu.make_async_copy(down_part(own), down_half(z, y), loc.at[1])
    load_gain = pltpu.make_async_copy(gain, gv, loc.at[2])
    load_tok = [pltpu.make_async_copy(
        tokens.at[pl.ds(pl.multiple_of(h * half, half), half)], tokv.at[h], loc.at[3 + i])
        for i, h in enumerate((c, 1 - c))]
    load_up.start()
    load_gain.start()
    for copy in load_tok:
        copy.start()
    load_down.start()
    pl.semaphore_wait(barrier, 3 + jnp.where(has_above, 1, 0) + jnp.where(has_below, 1, 0))

    up_order = (0, 1, 2)
    swap_up = [remote(up_part(x * 2 + 1 - y, k, 1), up_slot(z, 2 * y + k), w_s.at[0], w_r.at[k], to_y)
               for k in range(2)]
    swap_down = remote(down_part(x * 2 + 1 - y), down_half(z, y), w_s.at[1], w_r.at[2], to_y)

    def hop(w, upward, zz, p):
        slot, r = ((up_piece, zu_r), (down_slot, zd_r))[w]
        return remote(slot(zz, p), slot(zz, p), z_s.at[0 if upward else 1, zz],
                      r.at[zz, p], above if upward else below)

    def send(w, zz, p):
        @pl.when(jnp.logical_and(has_above, zz <= z))
        def _():
            hop(w, True, zz, p).start()

        @pl.when(jnp.logical_and(has_below, zz >= z))
        def _():
            hop(w, False, zz, p).start()

    def sent(zz):
        both = U.at[pl.ds(0, 2)]

        @pl.when(jnp.logical_and(has_above, zz <= z))
        def _():
            remote(both, both, z_s.at[0, zz], zu_r.at[0, 0], above).wait_send()

        @pl.when(jnp.logical_and(has_below, zz >= z))
        def _():
            remote(both, both, z_s.at[1, zz], zu_r.at[0, 0], below).wait_send()

    def relay(w, s, p):
        zz = order(s)

        @pl.when(inner)
        def _():
            hop(w, True, zz, p).wait_recv()
        send(w, zz, p)

    def arrived(w, s, p):
        @pl.when(edge)
        def _():
            hop(w, True, order(s), p).wait_recv()

    few = half // CHUNKS

    def piece(q, r):
        return T.at[:, q, c, pl.ds(r * few, few)]

    def tok(kind, r):
        if kind < 2:
            src, dev = piece(own, r), (to_a, to_b)[kind]
        elif kind == 2:
            flip = jnp.logical_and(c == 0, r in FORWARD_A)
            src = piece(jnp.where(flip, q_b, q_a), r)
            dev = {"rep": jnp.where(flip, ax, bx), "fs": z * 2 + jnp.where(flip, ay, by)}
        else:
            src, dev = piece((q_a, q_b, q_ab)[kind - 3], r), to_c
        land = tok_r.at[kind, r] if kind < 3 else cor_r.at[kind - 3]
        return remote(src, src, tok_s.at[0], land, dev)

    def crossed(kind):
        q = T.at[:, (q_b, q_a, q_ab)[kind - 3], 1 - c]
        remote(q, q, tok_s.at[0], cor_r.at[kind - 3], to_c).wait_recv()

    def norm(h, first, last):
        step = 16

        @pl.loop(first // step, last // step)
        def _(i):
            r = pl.ds(pl.multiple_of(i * step, step), step)
            xf = tokv[h, r, :].astype(F32)
            inv = lax.rsqrt(jnp.mean(xf * xf, axis=-1, keepdims=True) + eps)
            normed = (xf * inv * gv[...]).astype(BF16)
            for k in range(nz):
                T[k, own, h, r, :] = normed[:, k * blk:(k + 1) * blk]

    def up_blocks(blocks, s):
        zz = order(s)

        @pl.loop(0, 2 * len(blocks))
        def _(i):
            q, h = blocks[0], i % 2
            for n in range(1, len(blocks)):
                q = jnp.where(i // 2 == n, blocks[n], q)
            term = jnp.dot(T[zz, q, h], U[zz], preferred_element_type=F32)
            if s > 0:
                term += acc[q, h]
            if s < nz - 1:
                acc[q, h] = term
            else:
                hid[q, h] = jnp.square(jnp.maximum(term, 0.0)).astype(BF16)

    load_up.wait()
    send(0, z, 0)
    for copy in swap_up:
        copy.start()
    load_gain.wait()
    load_tok[0].wait()
    for r in range(CHUNKS):
        norm(c, r * few, (r + 1) * few)
        tok(0, r).start()
        tok(1, r).start()
    load_tok[1].wait()
    norm(1 - c, 0, half)
    for k in range(2):
        swap_up[k].wait_recv()
        send(0, z, 1 + k)
    for p in up_order:
        for s in range(1, min(3, nz)):
            relay(0, s, p)
    up_blocks((own,), 0)
    rest = [(s, p) for s in range(3, nz) for p in up_order]
    for r in range(CHUNKS):
        for kind in range(2):
            tok(kind, r).wait_recv()
            tok(3 + kind, r).start()
        tok(2, r).start()
        for s, p in rest[r::CHUNKS]:
            relay(0, s, p)
    load_down.wait()
    swap_down.start()

    def send_half(p):
        @pl.when(p == 0)
        def _():
            send(1, z, 0)

        @pl.when(p == 1)
        def _():
            for j in range(1, len(parts)):
                send(1, z, j)

    send_half(y)

    def edge_up(s):
        for p in up_order:
            arrived(0, s, p)

    edge_up(1)
    up_blocks((own,), 1)
    crossed(3)
    crossed(4)
    up_blocks((q_a, q_b), 0)
    up_blocks((q_a, q_b), 1)
    for s in range(2, nz - 1):
        edge_up(s)
        up_blocks((own, q_a, q_b), s)

    @pl.when(inner)
    def _():
        up_blocks((own, q_a, q_b), nz - 1)
    for r in range(CHUNKS):
        tok(2, r).wait_recv()
        tok(5, r).start()
    crossed(5)
    for s in range(nz - 1):
        up_blocks((q_ab,), s)
    edge_up(nz - 1)

    @pl.when(inner)
    def _():
        up_blocks((q_ab,), nz - 1)

    @pl.when(edge)
    def _():
        up_blocks((own, q_a, q_b, q_ab), nz - 1)
    swap_down.wait_recv()
    send_half(1 - y)
    every = T.at[:, pl.ds(0, 3)]
    remote(every, every, tok_s.at[0], cor_r.at[0], to_c).wait_send()

    def cols(p):
        return pl.ds(*p)

    def step(s, p):
        return 2 * s + tag(p)

    def group(s, k):
        return k if s < nz - 1 else 4 + k

    def d2d(s, p):
        zz = order(s)
        return remote(T.at[zz, :, 1 - c, :, cols(p)], Pr.at[zz, :, :, cols(p)],
                      out_s.at[group(s, 0)], d_r.at[step(s, p)], to_c)

    def to_first(s, p, i):
        zz = order(s)
        return remote(T.at[zz, (q_a, q_ab)[i], c, :, cols(p)], Ar.at[zz, i, :, cols(p)],
                      out_s.at[group(s, 1)], (b_r, a_r)[i].at[step(s, p)], to_a)

    def to_second(s, p):
        zz = order(s)
        return remote(T.at[zz, q_b, c, :, cols(p)], Br.at[zz, :, cols(p)],
                      out_s.at[group(s, 2)], b_r.at[step(s, p)], to_b)

    def place(s, p):
        k = order(s) % (nz // 2)
        return (pl.ds(pl.multiple_of(c * half, half), half),
                pl.ds(pl.multiple_of(k * blk + p[0], part), p[1]))

    def finish(s, p):
        zz = order(s)
        return remote(T.at[zz, own, c, :, cols(p)], out.at[place(s, p)],
                      out_s.at[3], f_r.at[0], to_c)

    def tag(p):
        return 2 if p[0] > row else p[0] // row

    def mine(s):
        return order(s) // (nz // 2) == c

    def stage_a(s, p):
        zz = order(s)
        for h in (1 - c, c):
            @pl.loop(0, 4, unroll=4)
            def _(q):
                T[zz, q, h, :, cols(p)] = jnp.dot(
                    hid[q, h], Dn[zz, :, cols(p)], preferred_element_type=F32).astype(BF16)
            if h is not c:
                d2d(s, p).start()

    def stage_a_early(s, p):
        zz = order(s)
        for h in range(2):
            @pl.loop(0, 4, unroll=4)
            def _(q):
                acc[q, h, :, :p[1]] = jnp.dot(
                    hid[q, h, :, :deep], Dn[zz, :deep, cols(p)], preferred_element_type=F32)

    def stage_a_late(s, p):
        zz = order(s)
        for h in range(2):
            @pl.loop(0, 4, unroll=4)
            def _(q):
                T[zz, q, h, :, cols(p)] = (acc[q, h, :, :p[1]] + jnp.dot(
                    hid[q, h, :, deep:], Dn[zz, deep:, cols(p)], preferred_element_type=F32)).astype(BF16)

            @pl.when(c == 0)
            def _():
                gather_last(s, p, h).start()

    def side(h):
        px, py = (1 - x, y), (x, 1 - y)
        (ax, ay), (bx, by) = (px, py) if h == 0 else (py, px)
        return (ax * 2 + ay, bx * 2 + by, {"rep": ax, "fs": z * 2 + ay}, {"rep": bx, "fs": z * 2 + by})

    def gather_last(s, p, h):
        return remote(T.at[order(s), :, h, :, cols(p)], P2.at[h], e_s.at[h], e_r.at[h], to_c)

    def first_last(s, p, h, i):
        qa, _, dev, _ = side(h)
        return remote(T.at[order(s), (qa, q_ab)[i], h, :, cols(p)], A2.at[h, i],
                      e_s.at[2 + 2 * h + i], e_r.at[2 + 2 * h + i], dev)

    def second_last(s, p, h):
        _, qb, _, dev = side(h)
        return remote(T.at[order(s), qb, h, :, cols(p)], B2.at[h], e_s.at[6 + h], e_r.at[6 + h], dev)

    def out_last(s, p, h):
        return (pl.ds(h * half, half),
                pl.ds(pl.multiple_of(order(s) % (nz // 2) * blk + p[0], part), p[1]))

    def finish_last(s, p, h):
        return remote(T.at[order(s), own, h, :, cols(p)], out.at[out_last(s, p, h)],
                      e_s.at[8 + h], e_r.at[8 + h], to_c)

    def last_b(s, p):
        zz, k = order(s), cols(p)
        for h in range(2):
            gather_last(s, p, h).wait_recv()
            T[zz, q_ab, h, :, k] = (
                T[zz, q_ab, h, :, k].astype(F32) + P2[h, q_ab].astype(F32)).astype(BF16)
            first_last(s, p, h, 1).start()
            for i, q in enumerate(side(h)[:2]):
                T[zz, q, h, :, k] = (
                    T[zz, q, h, :, k].astype(F32) + P2[h, q].astype(F32)).astype(BF16)
                if i == 0:
                    first_last(s, p, h, 0).start()

    def last_c(s, p):
        zz, k = order(s), cols(p)
        for h in range(2):
            qb = side(h)[1]
            first_last(s, p, h, 1).wait_recv()
            T[zz, qb, h, :, k] = (
                T[zz, qb, h, :, k].astype(F32) + A2[h, 1].astype(F32)).astype(BF16)
            second_last(s, p, h).start()

    def last_d(s, p):
        zz, k = order(s), cols(p)
        for h in range(2):
            T[zz, own, h, :, k] = (
                T[zz, own, h, :, k].astype(F32) + P2[h, own].astype(F32)).astype(BF16)
        for h in range(2):
            first_last(s, p, h, 0).wait_recv()
            second_last(s, p, h).wait_recv()
            total = (tokv[h, :, pl.ds(pl.multiple_of(zz * blk + p[0], part), p[1])].astype(F32)
                     + T[zz, own, h, :, k].astype(F32) + A2[h, 0].astype(F32)
                     + B2[h].astype(F32)).astype(BF16)

            @pl.when(mine(s))
            def _():
                out[out_last(s, p, h)] = total

            @pl.when(jnp.logical_not(mine(s)))
            def _():
                T[zz, own, h, :, k] = total
                finish_last(s, p, h).start()

    def stage_b(s, p):
        zz, k = order(s), cols(p)
        d2d(s, p).wait_recv()
        for i, q in ((1, q_ab), (0, q_a), (2, q_b), (3, own)):
            T[zz, q, c, :, k] = (
                T[zz, q, c, :, k].astype(F32) + Pr[zz, q, :, k].astype(F32)).astype(BF16)
            if i < 2:
                to_first(s, p, i).start()

    def stage_c(s, p):
        zz, k = order(s), cols(p)
        to_first(s, p, 1).wait_recv()
        T[zz, q_b, c, :, k] = (
            T[zz, q_b, c, :, k].astype(F32) + Ar[zz, 1, :, k].astype(F32)).astype(BF16)
        to_second(s, p).start()

    def stage_d(s, p):
        zz, k = order(s), cols(p)
        two = Ar.at[zz, :, :, k]
        remote(two, two, out_s.at[1], b_r.at[step(s, p)], to_a).wait_recv()
        total = (tokv[c, :, pl.ds(pl.multiple_of(zz * blk + p[0], part), p[1])].astype(F32)
                 + T[zz, own, c, :, k].astype(F32) + Ar[zz, 0, :, k].astype(F32)
                 + Br[zz, :, k].astype(F32)).astype(BF16)

        @pl.when(mine(s))
        def _():
            out[place(s, p)] = total

        @pl.when(jnp.logical_not(mine(s)))
        def _():
            T[zz, own, c, :, k] = total
            finish(s, p).start()

    steps = [(s, p) for s in range(nz) for p in ((0, row), (row, row))]
    steps[-1:] = [(nz - 1, p[:2]) for p in parts[1:3]]
    needs = [[j for j in range(len(parts)) if p[0] <= parts[j][0] < sum(p)] for _, p in steps]
    flat = [(s, j) for (s, _), js in zip(steps, needs) for j in js]
    relayed = set()

    def relay_until(s, j):
        for item in flat:
            if 0 < item[0] and item not in relayed and (item[0] < s or item[0] == s and item[1] <= j):
                relayed.add(item)
                relay(1, *item)

    last = len(steps) - 1

    def ready(n, js):
        s = steps[n][0]
        if s:
            for j in js:
                arrived(1, s, j)

    def plan(n):
        early = last - 3
        todo = [("c", n - 1)] if n and n - 1 != early else []
        todo.insert(0 if n == last - 1 else len(todo), ("b", n))
        if n > 1:
            todo.append(("d", n - 2))
        if n == early:
            todo.append(("c", n))
        return todo

    for n, (s, p) in enumerate(steps):
        first = tag(p) == 0
        if s == 1:
            for j in needs[n]:
                relay(1, 1, j)
                relay(1, 2, j)
            relayed.update((k, j) for k in (1, 2) for j in needs[n])
        elif 1 < s and n < last:
            relay_until(*((s, needs[n][-1]) if first or s == nz - 1 else (s + 1, 0)))
        if n < last:
            ready(n, needs[n])
            stage_a(s, p)
        else:
            for j, stage in zip(needs[n], (stage_a_early, stage_a_late)):
                relay_until(s, j)
                ready(n, (j,))
                stage(s, p)
        if n == last:
            break
        for kind, m in plan(n):
            {"b": stage_b, "c": stage_c, "d": stage_d}[kind](*steps[m])

    @pl.when(c == 1)
    def _():
        last_b(*steps[last])
    stage_c(*steps[last - 1])
    stage_d(*steps[last - 2])

    @pl.when(c == 1)
    def _():
        last_c(*steps[last])
    stage_d(*steps[last - 1])

    @pl.when(c == 1)
    def _():
        last_d(*steps[last])
    for zz in range(nz):
        sent(zz)
    ups = up_slot(0, 0, 2)
    remote(ups, ups, w_s.at[0], w_r.at[0], to_y).wait_send()
    swap_down.wait_send()

    def all_sent(ref, k):
        remote(ref, ref, out_s.at[k], d_r.at[0], to_c).wait_send()

    for k, ref in enumerate((Pr, Ar, Br)):
        all_sent(ref.at[pl.ds(0, nz - 1)], k)
        lead = (0,) + (slice(None),) * (len(ref.shape) - 2)
        all_sent(ref.at[(*lead, pl.ds(0, blk - part))], 4 + k)
    far = mine(nz - 1)
    most = out.at[pl.ds(0, half), pl.ds(0, (nz // 2) * blk - part)]
    full = out.at[pl.ds(0, half)]

    @pl.when(far)
    def _():
        all_sent(full, 3)
        remote(most, most, out_s.at[3], f_r.at[0], to_c).wait_recv()

    @pl.when(jnp.logical_not(far))
    def _():
        all_sent(most, 3)
        remote(full, full, out_s.at[3], f_r.at[0], to_c).wait_recv()

    end = steps[last]
    for h in range(2):
        @pl.when(c == 0)
        def _():
            gather_last(*end, h).wait_send()

        @pl.when(c == 1)
        def _():
            for i in range(2):
                first_last(*end, h, i).wait_send()
            second_last(*end, h).wait_send()

        @pl.when(jnp.logical_and(c == 1, jnp.logical_not(far)))
        def _():
            finish_last(*end, h).wait_send()

        @pl.when(jnp.logical_and(c == 0, far))
        def _():
            finish_last(*end, h).wait_recv()


def fused(nz, tokens, gain, up, down):
    rows, d = tokens.shape
    wide = up.shape[1] // 4
    half, blk = rows // 2, d // nz
    sem = pltpu.SemaphoreType.DMA
    return pl.pallas_call(
        functools.partial(kernel, nz, 1e-06),
        out_shape=pltpu.VMEM((rows, d // 2), BF16),
        in_specs=[pl.BlockSpec(memory_space=pl.ANY)] * 4,
        out_specs=pl.BlockSpec(memory_space=pltpu.VMEM),
        scratch_shapes=[
            pltpu.VMEM((nz, 4, 2, half, blk), BF16),
            pltpu.VMEM((4, 2, half, wide), F32),
            pltpu.VMEM((4, 2, half, wide), BF16),
            pltpu.VMEM((nz, blk, wide), BF16),
            pltpu.VMEM((nz, wide, blk), BF16),
            pltpu.VMEM((nz, 4, half, blk), BF16),
            pltpu.VMEM((nz, 2, half, blk), BF16),
            pltpu.VMEM((nz, half, blk), BF16),
            pltpu.VMEM((2, 4, half, blk // 4), BF16),
            pltpu.VMEM((2, 2, half, blk // 4), BF16),
            pltpu.VMEM((2, half, blk // 4), BF16),
            pltpu.VMEM((2, half, d), BF16),
            pltpu.VMEM((1, d), F32),
            sem((5,)), sem((1,)), sem((3, CHUNKS)), sem((3,)), sem((2,)), sem((3,)), sem((2, nz)),
            sem((nz, 3)), sem((nz, 4)), sem((2 * nz + 1,)), sem((2 * nz + 1,)), sem((2 * nz + 1,)),
            sem((7,)), sem((1,)), sem((10,)), sem((10,)),
        ],
        compiler_params=pltpu.CompilerParams(
            collective_id=0, has_side_effects=True, vmem_limit_bytes=58 * 2**20),
    )(tokens, gain.reshape(1, d), up, down)


def spread(normed, up_weight, down_weight):
    n_rep = lax.axis_size("rep")
    rep = lax.axis_index("rep")
    ff = up_weight.shape[1] // n_rep
    up = lax.all_gather(
        lax.dynamic_slice_in_dim(up_weight, rep * ff, ff, 1), "fs", axis=0, tiled=True)
    down = lax.all_gather(
        lax.dynamic_slice_in_dim(down_weight, rep * ff, ff, 0), "fs", axis=1, tiled=True)
    normed = lax.all_gather(normed, "rep", axis=0, tiled=True)
    pre = jnp.dot(normed, up, preferred_element_type=F32)
    hidden = jnp.square(jax.nn.relu(pre)).astype(BF16)
    terms = jnp.dot(hidden, down, preferred_element_type=F32).astype(BF16)
    summed = lax.psum_scatter(terms, "tp", scatter_dimension=1, tiled=True)
    return lax.psum_scatter(summed, "rep", scatter_dimension=0, tiled=True)


def local(tokens, norm_gain, up_weight, down_weight):
    n_rep, n_fs, n_tp = (lax.axis_size(a) for a in ("rep", "fs", "tp"))
    if n_rep == 2 and n_tp == 2 and n_fs % 4 == 0:
        got = fused(n_fs // 2, tokens, norm_gain, up_weight, down_weight)
        return got
    xf = tokens.astype(F32)
    inv_rms = lax.rsqrt(jnp.mean(xf * xf, axis=-1, keepdims=True) + 1e-06)
    normed = (xf * inv_rms * norm_gain).astype(BF16)
    summed = spread(normed, up_weight, down_weight).astype(F32)
    width = summed.shape[1]
    own_cols = lax.dynamic_slice_in_dim(xf, lax.axis_index("tp") * width, width, 1)
    return (own_cols + summed).astype(BF16)


def solution(mesh):
    placed = (P(("rep", "fs"), None), P(), P("fs", "tp"), P("tp", "fs"))
    return jax.shard_map(
        local, mesh=mesh, in_specs=placed, out_specs=P(("rep", "fs"), "tp"), check_vma=False
    )
```

```python
import functools

import jax
import jax.numpy as jnp
from jax import lax
from jax.experimental import pallas as pl
from jax.experimental.pallas import tpu as pltpu
from jax.sharding import PartitionSpec as P

MESH = pl.DeviceIdType.MESH
F32 = jnp.float32
BF16 = jnp.bfloat16


CHUNKS = 4
FORWARD_A = (3,)
EARLY_FROM = 5
SWAP = True
DEEP = 2


def kernel(nz, eps, tokens, gain, up, down, out, T, acc, hid, U, Dn, Pr, Ar, Br, P2, A2, B2, tokv, gv, loc,
           tok_s, tok_r, cor_r, w_s, w_r, z_s, zu_r, zd_r, d_r, a_r, b_r, out_s, f_r,
           e_s, e_r):
    x, f, c = lax.axis_index("rep"), lax.axis_index("fs"), lax.axis_index("tp")
    z, y = f // 2, f % 2
    half, blk = T.shape[3], T.shape[4]
    wide = U.shape[2]
    row = blk // 2
    sub = row // 2
    own = x * 2 + y
    ax, ay = (x + 1 - c) % 2, (y + c) % 2
    bx, by = (x + c) % 2, (y + 1 - c) % 2
    q_a, q_b, q_ab = ax * 2 + ay, bx * 2 + by, (1 - x) * 2 + 1 - y
    to_a = {"rep": ax, "fs": z * 2 + ay}
    to_b = {"rep": bx, "fs": z * 2 + by}
    to_y = {"fs": z * 2 + 1 - y}
    to_x = {"rep": 1 - x}
    to_c = {"tp": 1 - c}
    above = {"fs": jnp.minimum(z + 1, nz - 1) * 2 + y}
    below = {"fs": jnp.maximum(z - 1, 0) * 2 + y}
    has_above, has_below = z < nz - 1, z > 0
    inner = jnp.logical_and(has_above, has_below)
    edge = jnp.logical_not(inner)

    def remote(src, dst, s, r, dev):
        return pltpu.make_async_remote_copy(
            src_ref=src, dst_ref=dst, send_sem=s, recv_sem=r, device_id=dev, device_id_type=MESH)

    def order(s):
        m = jnp.minimum(z, nz - 1 - z)
        near = z - (s + 1) // 2 if s % 2 else z + s // 2
        far = jnp.where(z < nz - 1 - z, s, nz - 1 - s)
        return jnp.where(s <= 2 * m, near, far)

    barrier = pltpu.get_barrier_semaphore()
    for dev in (to_x, to_y, to_c):
        pl.semaphore_signal(barrier, inc=1, device_id=dev, device_id_type=MESH)

    @pl.when(has_above)
    def _():
        pl.semaphore_signal(barrier, inc=1, device_id=above, device_id_type=MESH)

    @pl.when(has_below)
    def _():
        pl.semaphore_signal(barrier, inc=1, device_id=below, device_id_type=MESH)

    def up_part(q, k, n):
        return up.at[pl.ds(k * sub, n * sub), pl.ds(pl.multiple_of(q * wide, wide), wide)]

    def down_part(q):
        return down.at[pl.ds(pl.multiple_of(q * wide, wide), wide)]

    part = row // 2
    deep = wide * DEEP // 4
    parts = ((0, row, 0, wide), (row, part, 0, wide), (row + part, part, 0, deep),
             (row + part, part, deep, wide - deep))

    def up_slot(zz, p, n=1):
        return U.at[zz, pl.ds(pl.multiple_of(p * sub, sub), n * sub)]

    def up_piece(zz, p):
        return up_slot(zz, 2 * y, 2) if p == 0 else up_slot(zz, 2 * (1 - y) + p - 1)

    def down_half(zz, p):
        return Dn.at[zz, :, pl.ds(pl.multiple_of(p * row, row), row)]

    def down_slot(zz, j):
        return Dn.at[zz, pl.ds(*parts[j][2:]), pl.ds(*parts[j][:2])]

    load_up = pltpu.make_async_copy(up_part(own, 0, 2), up_slot(z, 2 * y, 2), loc.at[0])
    load_down = pltpu.make_async_copy(down_part(own), down_half(z, y), loc.at[1])
    load_gain = pltpu.make_async_copy(gain, gv, loc.at[2])
    load_tok = [pltpu.make_async_copy(
        tokens.at[pl.ds(pl.multiple_of(h * half, half), half)], tokv.at[h], loc.at[3 + i])
        for i, h in enumerate((c, 1 - c))]
    load_up.start()
    load_gain.start()
    for copy in load_tok:
        copy.start()
    load_down.start()
    pl.semaphore_wait(barrier, 3 + jnp.where(has_above, 1, 0) + jnp.where(has_below, 1, 0))

    up_order = (0, 1, 2)
    swap_up = [remote(up_part(x * 2 + 1 - y, k, 1), up_slot(z, 2 * y + k), w_s.at[0], w_r.at[k], to_y)
               for k in range(2)]
    swap_down = remote(down_part(x * 2 + 1 - y), down_half(z, y), w_s.at[1], w_r.at[2], to_y)

    def hop(w, upward, zz, p):
        slot, r = ((up_piece, zu_r), (down_slot, zd_r))[w]
        return remote(slot(zz, p), slot(zz, p), z_s.at[0 if upward else 1, zz],
                      r.at[zz, p], above if upward else below)

    def send(w, zz, p):
        @pl.when(jnp.logical_and(has_above, zz <= z))
        def _():
            hop(w, True, zz, p).start()

        @pl.when(jnp.logical_and(has_below, zz >= z))
        def _():
            hop(w, False, zz, p).start()

    def sent(zz):
        both = U.at[pl.ds(0, 2)]

        @pl.when(jnp.logical_and(has_above, zz <= z))
        def _():
            remote(both, both, z_s.at[0, zz], zu_r.at[0, 0], above).wait_send()

        @pl.when(jnp.logical_and(has_below, zz >= z))
        def _():
            remote(both, both, z_s.at[1, zz], zu_r.at[0, 0], below).wait_send()

    def relay(w, s, p):
        zz = order(s)

        @pl.when(inner)
        def _():
            hop(w, True, zz, p).wait_recv()
        send(w, zz, p)

    def arrived(w, s, p):
        @pl.when(edge)
        def _():
            hop(w, True, order(s), p).wait_recv()

    few = half // CHUNKS

    def piece(q, r):
        return T.at[:, q, c, pl.ds(r * few, few)]

    def tok(kind, r):
        if kind < 2:
            src, dev = piece(own, r), (to_a, to_b)[kind]
        elif kind == 2:
            flip = jnp.logical_and(c == 0, r in FORWARD_A)
            src = piece(jnp.where(flip, q_b, q_a), r)
            dev = {"rep": jnp.where(flip, ax, bx), "fs": z * 2 + jnp.where(flip, ay, by)}
        else:
            src, dev = piece((q_a, q_b, q_ab)[kind - 3], r), to_c
        land = tok_r.at[kind, r] if kind < 3 else cor_r.at[kind - 3]
        return remote(src, src, tok_s.at[0], land, dev)

    def crossed(kind):
        q = T.at[:, (q_b, q_a, q_ab)[kind - 3], 1 - c]
        remote(q, q, tok_s.at[0], cor_r.at[kind - 3], to_c).wait_recv()

    def norm(h, first, last):
        step = 16

        @pl.loop(first // step, last // step)
        def _(i):
            r = pl.ds(pl.multiple_of(i * step, step), step)
            xf = tokv[h, r, :].astype(F32)
            inv = lax.rsqrt(jnp.mean(xf * xf, axis=-1, keepdims=True) + eps)
            normed = (xf * inv * gv[...]).astype(BF16)
            for k in range(nz):
                T[k, own, h, r, :] = normed[:, k * blk:(k + 1) * blk]

    def up_blocks(blocks, s):
        zz = order(s)

        @pl.loop(0, 2 * len(blocks))
        def _(i):
            q, h = blocks[0], i % 2
            for n in range(1, len(blocks)):
                q = jnp.where(i // 2 == n, blocks[n], q)
            term = jnp.dot(T[zz, q, h], U[zz], preferred_element_type=F32)
            if s > 0:
                term += acc[q, h]
            if s < nz - 1:
                acc[q, h] = term
            else:
                hid[q, h] = jnp.square(jnp.maximum(term, 0.0)).astype(BF16)

    load_up.wait()
    send(0, z, 0)
    for copy in swap_up:
        copy.start()
    load_gain.wait()
    load_tok[0].wait()
    for r in range(CHUNKS):
        norm(c, r * few, (r + 1) * few)
        tok(0, r).start()
        tok(1, r).start()
    load_tok[1].wait()
    norm(1 - c, 0, half)
    for k in range(2):
        swap_up[k].wait_recv()
        send(0, z, 1 + k)
    for p in up_order:
        for s in range(1, min(3, nz)):
            relay(0, s, p)
    up_blocks((own,), 0)
    rest = [(s, p) for s in range(3, nz) for p in up_order]
    for r in range(CHUNKS):
        for kind in range(2):
            tok(kind, r).wait_recv()
            tok(3 + kind, r).start()
        tok(2, r).start()
        for s, p in rest[r::CHUNKS]:
            relay(0, s, p)
    load_down.wait()
    swap_down.start()

    def send_half(p):
        @pl.when(p == 0)
        def _():
            send(1, z, 0)

        @pl.when(p == 1)
        def _():
            for j in range(1, len(parts)):
                send(1, z, j)

    send_half(y)

    def edge_up(s):
        for p in up_order:
            arrived(0, s, p)

    edge_up(1)
    up_blocks((own,), 1)
    crossed(3)
    crossed(4)
    up_blocks((q_a, q_b), 0)
    up_blocks((q_a, q_b), 1)
    for s in range(2, nz - 1):
        edge_up(s)
        up_blocks((own, q_a, q_b), s)

    @pl.when(inner)
    def _():
        up_blocks((own, q_a, q_b), nz - 1)
    for r in range(CHUNKS):
        tok(2, r).wait_recv()
        tok(5, r).start()
    crossed(5)
    for s in range(nz - 1):
        up_blocks((q_ab,), s)
    edge_up(nz - 1)

    @pl.when(inner)
    def _():
        up_blocks((q_ab,), nz - 1)

    @pl.when(edge)
    def _():
        up_blocks((own, q_a, q_b, q_ab), nz - 1)
    swap_down.wait_recv()
    send_half(1 - y)
    every = T.at[:, pl.ds(0, 3)]
    remote(every, every, tok_s.at[0], cor_r.at[0], to_c).wait_send()

    def cols(p):
        return pl.ds(*p)

    def step(s, p):
        return 2 * s + tag(p)

    def group(s, k):
        return k if s < nz - 1 else 4 + k

    def d2d(s, p):
        zz = order(s)
        return remote(T.at[zz, :, 1 - c, :, cols(p)], Pr.at[zz, :, :, cols(p)],
                      out_s.at[group(s, 0)], d_r.at[step(s, p)], to_c)

    def to_first(s, p, i):
        zz = order(s)
        return remote(T.at[zz, (q_a, q_ab)[i], c, :, cols(p)], Ar.at[zz, i, :, cols(p)],
                      out_s.at[group(s, 1)], (b_r, a_r)[i].at[step(s, p)], to_a)

    def to_second(s, p):
        zz = order(s)
        return remote(T.at[zz, q_b, c, :, cols(p)], Br.at[zz, :, cols(p)],
                      out_s.at[group(s, 2)], b_r.at[step(s, p)], to_b)

    def place(s, p):
        k = order(s) % (nz // 2)
        return (pl.ds(pl.multiple_of(c * half, half), half),
                pl.ds(pl.multiple_of(k * blk + p[0], part), p[1]))

    def finish(s, p):
        zz = order(s)
        return remote(T.at[zz, own, c, :, cols(p)], out.at[place(s, p)],
                      out_s.at[3], f_r.at[0], to_c)

    def tag(p):
        return 2 if p[0] > row else p[0] // row

    def mine(s):
        return order(s) // (nz // 2) == c

    def stage_a(s, p):
        zz = order(s)
        for h in (1 - c, c):
            @pl.loop(0, 4, unroll=4)
            def _(q):
                T[zz, q, h, :, cols(p)] = jnp.dot(
                    hid[q, h], Dn[zz, :, cols(p)], preferred_element_type=F32).astype(BF16)
            if h is not c:
                d2d(s, p).start()

    def stage_a_early(s, p):
        zz = order(s)
        for h in range(2):
            @pl.loop(0, 4, unroll=4)
            def _(q):
                acc[q, h, :, :p[1]] = jnp.dot(
                    hid[q, h, :, :deep], Dn[zz, :deep, cols(p)], preferred_element_type=F32)

    q_x, q_y = (1 - x) * 2 + y, x * 2 + 1 - y

    def stage_a_late(s, p):
        zz = order(s)
        for i, q in enumerate((q_ab, q_x, q_y, own)):
            for h in range(2):
                T[zz, q, h, :, cols(p)] = (acc[q, h, :, :p[1]] + jnp.dot(
                    hid[q, h, :, deep:], Dn[zz, deep:, cols(p)], preferred_element_type=F32)).astype(BF16)

            @pl.when(c == 0)
            def _():
                gather_last(s, p, q, i).start()

    def side(h):
        px, py = (1 - x, y), (x, 1 - y)
        (ax, ay), (bx, by) = (px, py) if h == 0 else (py, px)
        return (ax * 2 + ay, bx * 2 + by, {"rep": ax, "fs": z * 2 + ay}, {"rep": bx, "fs": z * 2 + by})

    def gather_last(s, p, q, i):
        return remote(T.at[order(s), q, :, :, cols(p)], P2.at[i], e_s.at[0], e_r.at[i], to_c)

    def first_last(s, p, h, i):
        qa, _, dev, _ = side(h)
        return remote(T.at[order(s), (qa, q_ab)[i], h, :, cols(p)], A2.at[h, i],
                      e_s.at[1], e_r.at[4 + h if i else 6 + h], dev)

    def second_last(s, p, h):
        _, qb, _, dev = side(h)
        return remote(T.at[order(s), qb, h, :, cols(p)], B2.at[h], e_s.at[2], e_r.at[6 + h], dev)

    def out_last(s, p, h):
        return (pl.ds(h * half, half),
                pl.ds(pl.multiple_of(order(s) % (nz // 2) * blk + p[0], part), p[1]))

    def finish_last(s, p, h):
        return remote(T.at[order(s), own, h, :, cols(p)], out.at[out_last(s, p, h)],
                      e_s.at[3], e_r.at[8], to_c)

    def join_last(s, p, q, i):
        zz, k = order(s), cols(p)
        gather_last(s, p, q, i).wait_recv()
        for h in range(2):
            T[zz, q, h, :, k] = (
                T[zz, q, h, :, k].astype(F32) + P2[i, h].astype(F32)).astype(BF16)

    def last_b(s, p):
        join_last(s, p, q_ab, 0)
        first_last(s, p, 0, 1).start()
        first_last(s, p, 1, 1).start()
        join_last(s, p, q_x, 1)
        first_last(s, p, 0, 0).start()
        join_last(s, p, q_y, 2)
        first_last(s, p, 1, 0).start()
        join_last(s, p, own, 3)

    def last_c(s, p):
        zz, k = order(s), cols(p)
        for h in range(2):
            qb = side(h)[1]
            first_last(s, p, h, 1).wait_recv()
            T[zz, qb, h, :, k] = (
                T[zz, qb, h, :, k].astype(F32) + A2[h, 1].astype(F32)).astype(BF16)
            second_last(s, p, h).start()

    def last_d(s, p):
        zz, k = order(s), cols(p)
        for h in range(2):
            pair = A2.at[h]
            remote(pair, pair, e_s.at[1], e_r.at[6 + h], to_c).wait_recv()
            total = (tokv[h, :, pl.ds(pl.multiple_of(zz * blk + p[0], part), p[1])].astype(F32)
                     + T[zz, own, h, :, k].astype(F32) + A2[h, 0].astype(F32)
                     + B2[h].astype(F32)).astype(BF16)

            @pl.when(mine(s))
            def _():
                out[out_last(s, p, h)] = total

            @pl.when(jnp.logical_not(mine(s)))
            def _():
                T[zz, own, h, :, k] = total
                finish_last(s, p, h).start()

    def stage_b(s, p):
        zz, k = order(s), cols(p)
        d2d(s, p).wait_recv()
        for i, q in ((1, q_ab), (0, q_a), (2, q_b), (3, own)):
            T[zz, q, c, :, k] = (
                T[zz, q, c, :, k].astype(F32) + Pr[zz, q, :, k].astype(F32)).astype(BF16)
            if i < 2:
                to_first(s, p, i).start()

    def stage_c(s, p):
        zz, k = order(s), cols(p)
        to_first(s, p, 1).wait_recv()
        T[zz, q_b, c, :, k] = (
            T[zz, q_b, c, :, k].astype(F32) + Ar[zz, 1, :, k].astype(F32)).astype(BF16)
        to_second(s, p).start()

    def stage_d(s, p):
        zz, k = order(s), cols(p)
        two = Ar.at[zz, :, :, k]
        remote(two, two, out_s.at[1], b_r.at[step(s, p)], to_a).wait_recv()
        total = (tokv[c, :, pl.ds(pl.multiple_of(zz * blk + p[0], part), p[1])].astype(F32)
                 + T[zz, own, c, :, k].astype(F32) + Ar[zz, 0, :, k].astype(F32)
                 + Br[zz, :, k].astype(F32)).astype(BF16)

        @pl.when(mine(s))
        def _():
            out[place(s, p)] = total

        @pl.when(jnp.logical_not(mine(s)))
        def _():
            T[zz, own, c, :, k] = total
            finish(s, p).start()

    steps = [(s, p) for s in range(nz) for p in ((0, row), (row, row))]
    steps[-1:] = [(nz - 1, p[:2]) for p in parts[1:3]]
    needs = [[j for j in range(len(parts)) if p[0] <= parts[j][0] < sum(p)] for _, p in steps]
    flat = [(s, j) for (s, _), js in zip(steps, needs) for j in js]
    relayed = set()

    def relay_until(s, j):
        for item in flat:
            if 0 < item[0] and item not in relayed and (item[0] < s or item[0] == s and item[1] <= j):
                relayed.add(item)
                relay(1, *item)

    last = len(steps) - 1

    def ready(n, js):
        s = steps[n][0]
        if s:
            for j in js:
                arrived(1, s, j)

    def plan(n):
        early = range(EARLY_FROM, last - 2)
        todo = [("c", n - 1)] if n and n - 1 not in early else []
        todo.insert(0 if n == last - 1 and SWAP else len(todo), ("b", n))
        if n > 1:
            todo.append(("d", n - 2))
        if n in early:
            todo.append(("c", n))
        return todo

    for n, (s, p) in enumerate(steps):
        first = tag(p) == 0
        if s == 1:
            for j in needs[n]:
                relay(1, 1, j)
                relay(1, 2, j)
            relayed.update((k, j) for k in (1, 2) for j in needs[n])
        elif 1 < s and n < last:
            relay_until(*((s, needs[n][-1]) if first or s == nz - 1 else (s + 1, 0)))
        if n < last:
            ready(n, needs[n])
            stage_a(s, p)
        else:
            for j, stage in zip(needs[n], (stage_a_early, stage_a_late)):
                relay_until(s, j)
                ready(n, (j,))
                stage(s, p)
        if n == last:
            break
        for kind, m in plan(n):
            {"b": stage_b, "c": stage_c, "d": stage_d}[kind](*steps[m])

    @pl.when(c == 1)
    def _():
        last_b(*steps[last])
    stage_c(*steps[last - 1])
    stage_d(*steps[last - 2])

    @pl.when(c == 1)
    def _():
        last_c(*steps[last])
    stage_d(*steps[last - 1])

    @pl.when(c == 1)
    def _():
        last_d(*steps[last])
    for zz in range(nz):
        sent(zz)
    ups = up_slot(0, 0, 2)
    remote(ups, ups, w_s.at[0], w_r.at[0], to_y).wait_send()
    swap_down.wait_send()

    def all_sent(ref, k):
        remote(ref, ref, out_s.at[k], d_r.at[0], to_c).wait_send()

    for k, ref in enumerate((Pr, Ar, Br)):
        all_sent(ref.at[pl.ds(0, nz - 1)], k)
        lead = (0,) + (slice(None),) * (len(ref.shape) - 2)
        all_sent(ref.at[(*lead, pl.ds(0, blk - part))], 4 + k)
    far = mine(nz - 1)
    most = out.at[pl.ds(0, half), pl.ds(0, (nz // 2) * blk - part)]
    full = out.at[pl.ds(0, half)]

    @pl.when(far)
    def _():
        all_sent(full, 3)
        remote(most, most, out_s.at[3], f_r.at[0], to_c).wait_recv()

    @pl.when(jnp.logical_not(far))
    def _():
        all_sent(most, 3)
        remote(full, full, out_s.at[3], f_r.at[0], to_c).wait_recv()

    far_rows = P2.at[3]

    @pl.when(c == 0)
    def _():
        remote(P2, P2, e_s.at[0], e_r.at[0], to_c).wait_send()

    @pl.when(c == 1)
    def _():
        remote(A2, A2, e_s.at[1], e_r.at[0], to_c).wait_send()
        remote(B2, B2, e_s.at[2], e_r.at[0], to_c).wait_send()

    @pl.when(jnp.logical_and(c == 1, jnp.logical_not(far)))
    def _():
        remote(far_rows, far_rows, e_s.at[3], e_r.at[0], to_c).wait_send()

    @pl.when(jnp.logical_and(c == 0, far))
    def _():
        remote(far_rows, far_rows, e_s.at[3], e_r.at[8], to_c).wait_recv()


def fused(nz, tokens, gain, up, down):
    rows, d = tokens.shape
    wide = up.shape[1] // 4
    half, blk = rows // 2, d // nz
    sem = pltpu.SemaphoreType.DMA
    return pl.pallas_call(
        functools.partial(kernel, nz, 1e-06),
        out_shape=pltpu.VMEM((rows, d // 2), BF16),
        in_specs=[pl.BlockSpec(memory_space=pl.ANY)] * 4,
        out_specs=pl.BlockSpec(memory_space=pltpu.VMEM),
        scratch_shapes=[
            pltpu.VMEM((nz, 4, 2, half, blk), BF16),
            pltpu.VMEM((4, 2, half, wide), F32),
            pltpu.VMEM((4, 2, half, wide), BF16),
            pltpu.VMEM((nz, blk, wide), BF16),
            pltpu.VMEM((nz, wide, blk), BF16),
            pltpu.VMEM((nz, 4, half, blk), BF16),
            pltpu.VMEM((nz, 2, half, blk), BF16),
            pltpu.VMEM((nz, half, blk), BF16),
            pltpu.VMEM((4, 2, half, blk // 4), BF16),
            pltpu.VMEM((2, 2, half, blk // 4), BF16),
            pltpu.VMEM((2, half, blk // 4), BF16),
            pltpu.VMEM((2, half, d), BF16),
            pltpu.VMEM((1, d), F32),
            sem((5,)), sem((1,)), sem((3, CHUNKS)), sem((3,)), sem((2,)), sem((3,)), sem((2, nz)),
            sem((nz, 3)), sem((nz, 4)), sem((2 * nz,)), sem((2 * nz,)), sem((2 * nz,)),
            sem((7,)), sem((1,)), sem((4,)), sem((9,)),
        ],
        compiler_params=pltpu.CompilerParams(
            collective_id=0, has_side_effects=True, vmem_limit_bytes=58 * 2**20),
    )(tokens, gain.reshape(1, d), up, down)


def spread(normed, up_weight, down_weight):
    n_rep = lax.axis_size("rep")
    rep = lax.axis_index("rep")
    ff = up_weight.shape[1] // n_rep
    up = lax.all_gather(
        lax.dynamic_slice_in_dim(up_weight, rep * ff, ff, 1), "fs", axis=0, tiled=True)
    down = lax.all_gather(
        lax.dynamic_slice_in_dim(down_weight, rep * ff, ff, 0), "fs", axis=1, tiled=True)
    normed = lax.all_gather(normed, "rep", axis=0, tiled=True)
    pre = jnp.dot(normed, up, preferred_element_type=F32)
    hidden = jnp.square(jax.nn.relu(pre)).astype(BF16)
    terms = jnp.dot(hidden, down, preferred_element_type=F32).astype(BF16)
    summed = lax.psum_scatter(terms, "tp", scatter_dimension=1, tiled=True)
    return lax.psum_scatter(summed, "rep", scatter_dimension=0, tiled=True)


def local(tokens, norm_gain, up_weight, down_weight):
    n_rep, n_fs, n_tp = (lax.axis_size(a) for a in ("rep", "fs", "tp"))
    if n_rep == 2 and n_tp == 2 and n_fs % 4 == 0:
        got = fused(n_fs // 2, tokens, norm_gain, up_weight, down_weight)
        return got
    xf = tokens.astype(F32)
    inv_rms = lax.rsqrt(jnp.mean(xf * xf, axis=-1, keepdims=True) + 1e-06)
    normed = (xf * inv_rms * norm_gain).astype(BF16)
    summed = spread(normed, up_weight, down_weight).astype(F32)
    width = summed.shape[1]
    own_cols = lax.dynamic_slice_in_dim(xf, lax.axis_index("tp") * width, width, 1)
    return (own_cols + summed).astype(BF16)


def solution(mesh):
    placed = (P(("rep", "fs"), None), P(), P("fs", "tp"), P("tp", "fs"))
    return jax.shard_map(
        local, mesh=mesh, in_specs=placed, out_specs=P(("rep", "fs"), "tp"), check_vma=False
    )
```
